32 devices in a mesh: fs: 8 (over z, y), tp: 4 (over x, core).
Axes of the slice: x: 2, y: 2, z: 4, core: 2. Of those that a mesh axis runs over, the one named last changes fastest.
Arguments:
- resid: bfloat16 [12288, 2048], P(('fs', 'tp')), may hold values from -6 to 6
- norm1_gain: float32 [2048], replicated, may hold values from 0.1 to 1.9
- w_value: float32 [2048, 2048], P('fs', 'tp'), may hold values from -0.125 to 0.125
- w_gate: float32 [2048, 2048], P('fs', 'tp'), may hold values from -0.125 to 0.125
- value_scale: float32 [2048], replicated, may hold values from 0.3 to 3
- gate_scale: float32 [2048], replicated, may hold values from 0.5 to 3
- conv_taps: float32 [31, 2048], replicated, may hold values from -1 to 1
- conv_gain: float32 [2048], replicated, may hold values from 0.1 to 1.9
- w_point: float32 [2048, 2048], P('tp', 'fs'), may hold values from -0.125 to 0.125
- point_scale: float32 [2048], P('fs'), may hold values from 0.5 to 3
- norm2_gain: float32 [2048], replicated, may hold values from 0.1 to 1.9
- w_up: float32 [2048, 8192], P('fs', 'tp'), may hold values from -0.125 to 0.125
- up_scale: float32 [8192], P('tp'), may hold values from 0.5 to 1.5
- w_down: float32 [8192, 2048], P('tp', 'fs'), may hold values from -0.0625 to 0.0625
- down_scale: float32 [2048], P('fs'), may hold values from 0.3 to 1
Outputs:
- layer_out: bfloat16 [12288, 2048], P(('fs', 'tp'))
The draws below stay inside these ranges and needn't reach their ends.
All inputs are finite; a program needn't handle non-finite values.
Results may differ from the reference program's by a relative error of at most 0.015.
Values may be sent and summed in bfloat16 or wider, within the bound.
A program may use at most 128 MiB of HBM per device.

```python
import math
import jax
import jax.numpy as jnp
from jax import lax

D = 2048
CH = 2048
FF = 8192
KERNEL = 31
GROUPS = 4
LEN = 1536
TOKENS = 12288
N_TP = 4


def levels(stream_key, extent, shards, low, top_value):
    level = 1.0
    for position, shards_of in shards:
        heights = jax.random.uniform(jax.random.fold_in(jax.random.fold_in(stream_key, 6), position), (shards_of,), jnp.float32, low / len(shards), top_value / len(shards))
        level = level * jnp.repeat(jnp.exp(heights), extent[position] // shards_of).reshape((-1,) + (1,) * (len(extent) - 1 - position))
    return level


def noise(own_key, extent, scale, most, pieces=(), kind=jnp.bfloat16):
    entries = scale * jax.random.normal(own_key, extent, jnp.float32)
    if pieces:
        entries = entries * levels(own_key, extent, pieces, -0.22, 0.18)
    return jnp.clip(entries, -most, most).astype(kind)


def setup_inputs(seed: int = 0) -> dict:
    key_list = jax.random.split(jax.random.key(seed), 16)
    return {
        "resid": noise(key_list[0], (TOKENS, D), 1.0, 6.0, ((0, 32),)),
        "norm1_gain": jnp.clip(1.0 + 0.18 * jax.random.normal(key_list[1], (D,), jnp.float32), 0.1, 1.9),
        "w_value": noise(key_list[2], (D, CH), D ** -0.5, 0.125, ((0, 8), (1, 4)), jnp.float32),
        "w_gate": noise(key_list[3], (D, CH), D ** -0.5, 0.125, ((0, 8), (1, 4)), jnp.float32),
        "value_scale": jnp.clip(jnp.exp(jax.random.uniform(key_list[4], (CH,), jnp.float32, math.log(0.3), math.log(3.0))), 0.3, 3.0),
        "gate_scale": jnp.clip(jnp.exp(jax.random.uniform(key_list[5], (CH,), jnp.float32, math.log(0.5), math.log(3.0))), 0.5, 3.0),
        "conv_taps": noise(key_list[6], (KERNEL, CH), KERNEL ** -0.5, 1.0, (), jnp.float32),
        "conv_gain": jnp.clip(1.0 + 0.18 * jax.random.normal(key_list[7], (CH,), jnp.float32), 0.1, 1.9),
        "w_point": noise(key_list[8], (CH, D), CH ** -0.5, 0.125, ((0, 4), (1, 8)), jnp.float32),
        "point_scale": jnp.clip(jnp.exp(math.log(3.0) - 1.7917595 * jax.random.uniform(key_list[9], (D,), jnp.float32) ** levels(key_list[9], (D,), ((0, 8),), -0.2, 0.2)), 0.5, 3.0),
        "norm2_gain": jnp.clip(1.0 + 0.18 * jax.random.normal(key_list[10], (D,), jnp.float32), 0.1, 1.9),
        "w_up": noise(key_list[11], (D, FF), D ** -0.5, 0.125, ((0, 8), (1, 4)), jnp.float32),
        "up_scale": jnp.clip(jnp.exp(math.log(1.5) - 1.0986123 * jax.random.uniform(key_list[12], (FF,), jnp.float32) ** levels(key_list[12], (FF,), ((0, 4),), -0.2, 0.2)), 0.5, 1.5),
        "w_down": noise(key_list[13], (FF, D), FF ** -0.5, 0.0625, ((0, 4), (1, 8)), jnp.float32),
        "down_scale": jnp.clip(jnp.exp(math.log(1.0) - 1.2039728 * jax.random.uniform(key_list[14], (D,), jnp.float32) ** levels(key_list[14], (D,), ((0, 8),), -0.2, 0.2)), 0.3, 1.0),
    }


def rms_scaled(values, gain):
    data = values.astype(jnp.float32)
    return data * lax.rsqrt(lax.optimization_barrier(jnp.mean(data * data, axis=-1, keepdims=True)) + 1e-06) * gain

def reference(resid, norm1_gain, w_value, w_gate, value_scale, gate_scale, conv_taps, conv_gain, w_point, point_scale, norm2_gain, w_up, up_scale, w_down, down_scale):
    value_bf = w_value.astype(jnp.bfloat16)
    gate_bf = w_gate.astype(jnp.bfloat16)
    point_bf = w_point.astype(jnp.bfloat16)
    up_bf = w_up.astype(jnp.bfloat16)
    down_bf = w_down.astype(jnp.bfloat16)
    normed = rms_scaled(resid, norm1_gain).astype(jnp.bfloat16)
    value = jnp.dot(normed, value_bf, preferred_element_type=jnp.float32) * value_scale
    gate = jnp.dot(normed, gate_bf, preferred_element_type=jnp.float32) * gate_scale
    glu = (value * jax.nn.sigmoid(gate)).astype(jnp.bfloat16)
    reach = KERNEL // 2
    seqs = glu.reshape(-1, LEN, CH).astype(jnp.float32)
    padded = jnp.pad(seqs, ((0, 0), (reach, reach), (0, 0)))
    conv = jnp.zeros(seqs.shape, jnp.float32)
    for offset in range(KERNEL):
        conv = conv + conv_taps[offset] * padded[:, offset:offset + LEN]
    grouped = conv.reshape(-1, CH // GROUPS, GROUPS)
    gmean = lax.optimization_barrier(jnp.mean(grouped, axis=-2, keepdims=True))
    gsquare = lax.optimization_barrier(jnp.mean(grouped * grouped, axis=-2, keepdims=True))
    scaled = ((grouped - gmean) * lax.rsqrt(gsquare - gmean * gmean + 1e-05)).reshape(-1, CH) * conv_gain
    act = jax.nn.silu(scaled).astype(jnp.bfloat16)
    mixed = jnp.dot(act, point_bf, preferred_element_type=jnp.float32) * point_scale
    middle = (resid.astype(jnp.float32) + mixed).astype(jnp.bfloat16)
    normed2 = rms_scaled(middle, norm2_gain).astype(jnp.bfloat16)
    upper = jnp.dot(normed2, up_bf, preferred_element_type=jnp.float32) * up_scale
    hidden = jnp.square(jax.nn.relu(upper)).astype(jnp.bfloat16)
    block = FF // N_TP
    hid_blocks = jnp.transpose(hidden.reshape(hidden.shape[0], N_TP, block), (1, 0, 2))
    down_blocks = down_bf.reshape(N_TP, block, D)

    def add_block(total, pair):
        hid_block, down_block = pair
        partial_value = (jnp.dot(hid_block, down_block, preferred_element_type=jnp.float32) * down_scale).astype(jnp.bfloat16)
        partial_value = lax.optimization_barrier(partial_value)
        return (total + partial_value.astype(jnp.float32), None)
    total, _ = lax.scan(add_block, jnp.zeros((hidden.shape[0], D), jnp.float32), (hid_blocks, down_blocks))
    return (middle.astype(jnp.float32) + total).astype(jnp.bfloat16)
```

```python
import functools

import jax
import jax.numpy as jnp
from jax import lax
from jax.experimental import pallas as pl
from jax.experimental.pallas import tpu as pltpu
from jax.sharding import PartitionSpec as P

GROUPS = 4
CORES = 2
CHUNKS = 16
PIECES = 4
LANES = 128
PAD = 16
MESH = pl.DeviceIdType.MESH


def ring_at(q, count):
    q = lax.rem(q + 2 * count, count)
    high = q // (count // 2)
    return (1 - high) * 2 * q + high * (2 * (count - 1 - q) + 1)


def layer_kernel(
    n, count, group_width,
    resid_hbm, vg_hbm, pt_hbm, up_hbm, dn_hbm, gain1_ref, vs_ref, gs_ref, taps_ref, cgain_ref, gain2_ref, us_ref,
    out_ref,
    resid, tok1, tok2, vg, pt, up, dn, gl, cv, act, pb, near_in, far_in, theirs, st, st_in,
    load_sem, ring_send, ring_recv,
    g1fs, g1fr, g1ns, g1nr, sss, ssr, scns, scnr, scfs, scfr, g2fs, g2fr, g2ns, g2nr, mns, mnr, mfs, mfr,
):
    me = lax.axis_index("tp")
    core = lax.rem(me, CORES)
    chip = me // CORES
    chips = n // CORES
    other = CORES - 1 - core
    partner = chip * CORES + other
    seat = lax.axis_index("fs")
    odd = lax.rem(seat, 2)
    pos = (1 - odd) * (seat // 2) + odd * (count - 1 - seat // 2)
    right, left = ring_at(pos + 1, count), ring_at(pos - 1, count)
    rows, width = resid.shape
    seq = rows * n
    pieces = CHUNKS // n
    r = rows // pieces
    own_w = pt.shape[1]
    blocks = own_w // LANES
    db = pt.shape[2]
    hid = dn.shape[1]
    far_step = count // 2
    reach = taps_ref.shape[0] // 2
    f32 = jnp.float32

    def chip_core(c, k):
        return lax.rem(c + 2 * chips, chips) * CORES + k

    loads = [
        pltpu.make_async_copy(vg_hbm, vg.at[pl.ds(pl.multiple_of(seat * db, db), db)], load_sem.at[0]),
        pltpu.make_async_copy(resid_hbm, resid, load_sem.at[1]),
        pltpu.make_async_copy(pt_hbm, pt.at[seat], load_sem.at[2]),
        pltpu.make_async_copy(up_hbm, up.at[pl.ds(pl.multiple_of(seat * db, db), db)], load_sem.at[3]),
        pltpu.make_async_copy(dn_hbm, dn.at[0], load_sem.at[4]),
    ]
    for load in loads:
        load.start()
    barrier = pltpu.get_barrier_semaphore()
    for target in (left, right):
        pl.semaphore_signal(barrier, inc=1, device_id={"fs": target}, device_id_type=MESH)
    for d in range(1, n):
        pl.semaphore_signal(barrier, inc=1, device_id={"tp": lax.rem(me + d, n)}, device_id_type=MESH)
    pl.semaphore_wait(barrier, n + 1)

    VG, PT, UP, DN = range(4)

    def spot(a, s, k, clockwise):
        owner = ring_at(pos - s if clockwise else pos + s, count)
        if a in (VG, UP):
            step = db // PIECES
            return (vg if a == VG else up).at[pl.ds(pl.multiple_of(owner * db + k * step, step), step)]
        if a == PT:
            step = own_w // PIECES
            return pt.at[owner, pl.ds(pl.multiple_of(k * step, step), step)]
        step = hid // PIECES
        slot = lax.rem(s if clockwise else count - s, count)
        return dn.at[slot, pl.ds(pl.multiple_of(k * step, step), step)]

    def dn_dst(s, k, clockwise):
        step = hid // PIECES
        return dn.at[s if clockwise else count - s, pl.ds(pl.multiple_of(k * step, step), step)]

    def hop(a, s, k, clockwise):
        way = 0 if clockwise else 1
        src = spot(a, s - 1, k, clockwise)
        dst = dn_dst(s, k, clockwise) if a == DN else src
        return pltpu.make_async_remote_copy(
            src_ref=src, dst_ref=dst, send_sem=ring_send.at[a, way, s - 1, k], recv_sem=ring_recv.at[a, way, s - 1, k],
            device_id={"fs": right if clockwise else left}, device_id_type=MESH)

    def arrived(a, s, k, clockwise):
        way = 0 if clockwise else 1
        here = spot(a, s, k, clockwise)
        pltpu.make_async_remote_copy(
            src_ref=here, dst_ref=here, send_sem=ring_send.at[a, way, s - 1, k], recv_sem=ring_recv.at[a, way, s - 1, k],
            device_id={"fs": right if clockwise else left}, device_id_type=MESH).wait_recv()

    half = PIECES // 2
    full_items = (far_step - 1) * PIECES
    items = full_items + half

    def first_hops(a):
        for k in range(PIECES):
            for clockwise in (True, False):
                hop(a, 1, k, clockwise).start()

    def service(a, i):
        if isinstance(i, int) and i >= full_items:
            k = i - full_items
            arrived(a, far_step, k, True)
            arrived(a, far_step, k + half, False)
            return
        s, k = i // PIECES + 1, i % PIECES
        for clockwise in (True, False):
            arrived(a, s, k, clockwise)
            mine = k < half if clockwise else k >= half
            if isinstance(i, int):
                if s + 1 < far_step or mine:
                    hop(a, s + 1, k, clockwise).start()
            else:
                @pl.when(jnp.logical_or(s + 1 < far_step, mine))
                def _():
                    hop(a, s + 1, k, clockwise).start()

    done = [0, 0, 0, 0]

    def upto(a, q):
        q = q * items // 14
        for i in range(done[a], q):
            service(a, i)
            if i == full_items - 1 and a < DN:
                first_hops(a + 1)
        done[a] = max(done[a], q)

    loads[0].wait()
    first_hops(VG)

    loads[1].wait()

    def t1(owner, k):
        return tok1.at[pl.ds(pl.multiple_of(owner * rows + k * r, r), r)]

    def far1(d, k, owner, target):
        return pltpu.make_async_remote_copy(
            src_ref=t1(owner, k), dst_ref=t1(owner, k), send_sem=g1fs.at[d - 1, k], recv_sem=g1fr.at[d - 1, k],
            device_id={"tp": target}, device_id_type=MESH)

    def near1(d, k, owner):
        return pltpu.make_async_remote_copy(
            src_ref=t1(owner, k), dst_ref=t1(owner, k), send_sem=g1ns.at[d, k], recv_sem=g1nr.at[d, k],
            device_id={"tp": partner}, device_id_type=MESH)

    sub = 16
    for k in range(pieces):
        @pl.loop(0, r // sub)
        def _(t):
            at = k * r + t * sub
            data = resid[pl.ds(pl.multiple_of(at, sub), sub), :].astype(f32)
            scale = lax.rsqrt(jnp.mean(data * data, axis=-1, keepdims=True) + 1e-06)
            tok1[pl.ds(pl.multiple_of(me * rows + at, sub), sub), :] = (data * scale * gain1_ref[...]).astype(tok1.dtype)

        for d in range(1, chips):
            far1(d, k, me, chip_core(chip + d, core)).start()
        near1(0, k, me).start()
    for load in loads[2:]:
        load.wait()
    passed = 0
    for q in range(14):
        upto(VG, q + 1)
        while passed < pieces and (passed + 1) * 13 // pieces <= q + 1:
            for d in range(1, chips):
                owner = chip_core(chip - d, core)
                far1(d, passed, owner, partner).wait_recv()
                near1(d, passed, owner).start()
            passed += 1
    for k in range(pieces):
        for d in range(chips):
            near1(d, k, chip_core(chip - d, other)).wait_recv()

    gl[:, 0:PAD, :] = jnp.zeros((blocks, PAD, LANES), f32)
    gl[:, PAD + seq :, :] = jnp.zeros((blocks, PAD, LANES), f32)
    mine_w = pl.multiple_of(me * own_w, own_w)
    tile = 256
    tiles = seq // tile
    wide = 2 * LANES

    @pl.loop(0, tiles)
    def _(t):
        at = pl.multiple_of(t * tile, tile)
        for c in range(0, own_w, wide):
            lhs = tok1[pl.ds(at, tile), :]
            value = jnp.dot(lhs, vg[:, c : c + wide], preferred_element_type=f32)
            gate = jnp.dot(lhs, vg[:, own_w + c : own_w + c + wide], preferred_element_type=f32)
            value = value * vs_ref[:, pl.ds(mine_w + c, wide)]
            gate = gate * gs_ref[:, pl.ds(mine_w + c, wide)]
            glu = (value * jax.nn.sigmoid(gate)).astype(jnp.bfloat16).astype(f32)
            for b in range(wide // LANES):
                gl[c // LANES + b, pl.ds(PAD + at, tile), :] = glu[:, b * LANES : (b + 1) * LANES]

        @pl.when(jnp.logical_and(t >= 2, t < 2 + PIECES))
        def _():
            service(PT, t - 2)

    done[PT] = PIECES

    span = seq // CHUNKS
    lane = lax.broadcasted_iota(jnp.int32, (span, LANES), 1)
    st[...] = jnp.zeros(st.shape, f32)

    def spread(v, width_from):
        while width_from < LANES:
            v = v + pltpu.roll(v, width_from, 1)
            width_from *= 2
        return v

    @pl.loop(0, CHUNKS)
    def _(i):
        at = pl.multiple_of(i * span, span)
        total = jnp.zeros((span, LANES), f32)
        square = jnp.zeros((span, LANES), f32)
        for b in range(blocks):
            window = gl[b, pl.ds(at, span + 2 * PAD), :]
            lanes = pl.ds(mine_w + b * LANES, LANES)
            conv = None
            for phase in range(8):
                acc = None
                for a in range(4):
                    j = 8 * a + phase + reach - PAD
                    if j < 0 or j > 2 * reach:
                        continue
                    term = taps_ref[j : j + 1, lanes] * window[8 * a : 8 * a + span + 8]
                    acc = term if acc is None else acc + term
                if phase:
                    acc = pltpu.roll(acc, span + 8 - phase, 0)
                acc = acc[:span]
                conv = acc if conv is None else conv + acc
            cv[b, pl.ds(at, span), :] = conv
            total = total + conv
            square = square + conv * conv
        total = spread(total, GROUPS)
        square = spread(square, GROUPS)
        here = lane // (2 * GROUPS) == i
        st[...] = jnp.where(here, jnp.where(lane % (2 * GROUPS) < GROUPS, total, square), st[...])

        @pl.when(jnp.logical_and(i >= 6, i < 6 + 2 * PIECES))
        def _():
            service(PT, PIECES + i - 6)

    done[PT] = 3 * PIECES
    if full_items == 3 * PIECES:
        first_hops(UP)

    def stat(d):
        return pltpu.make_async_remote_copy(
            src_ref=st, dst_ref=st_in.at[d - 1], send_sem=sss.at[d - 1], recv_sem=ssr.at[d - 1],
            device_id={"tp": lax.rem(me + d, n)}, device_id_type=MESH)

    for d in range(1, n):
        stat(d).start()
    upto(PT, 14)
    for d in range(1, n):
        stat(d).wait_recv()
    for d in range(1, n):
        stat(d).wait_send()
    st_sum = st[...]
    for d in range(1, n):
        st_sum = st_sum + st_in[d - 1]
    st[...] = st_sum

    def scn(d, k):
        return pltpu.make_async_remote_copy(
            src_ref=pb.at[:, k, chip_core(chip + d, other)],
            dst_ref=near_in.at[:, k] if d == 0 else theirs.at[d - 1, :, k],
            send_sem=scns.at[d, k], recv_sem=scnr.at[d, k], device_id={"tp": partner}, device_id_type=MESH)

    def scf(d, k):
        return pltpu.make_async_remote_copy(
            src_ref=pb.at[:, k, chip_core(chip + d, core)], dst_ref=far_in.at[d - 1, :, k],
            send_sem=scfs.at[d - 1, k], recv_sem=scfr.at[d - 1, k],
            device_id={"tp": chip_core(chip + d, core)}, device_id_type=MESH)

    def mix(k):
        @pl.loop(0, n)
        def _(o):
            i = o * pieces + k
            here = lane // GROUPS
            stats = st[...]
            gmean = spread(jnp.where(here == 2 * i, stats, 0.0), GROUPS) / group_width
            gsquare = spread(jnp.where(here == 2 * i + 1, stats, 0.0), GROUPS) / group_width
            inv = lax.rsqrt(gsquare - gmean * gmean + 1e-05)
            for b in range(blocks):
                conv = cv[b, pl.ds(pl.multiple_of(i * span, span), span), :]
                scaled = (conv - gmean) * inv * cgain_ref[:, pl.ds(mine_w + b * LANES, LANES)]
                act[pl.ds(pl.multiple_of((k * n + o) * r, r), r), b * LANES : (b + 1) * LANES] = (
                    scaled / (1.0 + jnp.exp(-scaled))
                ).astype(act.dtype)

        @pl.loop(0, count)
        def _(j):
            part = jnp.dot(act[k * n * r : (k + 1) * n * r, :], pt[j], preferred_element_type=f32)
            pb[j, k] = part.astype(pb.dtype).reshape(n, r, db)

        for d in list(range(1, chips)) + [0]:
            scn(d, k).start()

    def mix_far(k):
        for d in range(1, chips):
            scn(d, k).wait_recv()
            owner = chip_core(chip + d, core)

            @pl.loop(0, count)
            def _(j):
                total = pb[j, k, owner].astype(f32) + theirs[d - 1, j, k].astype(f32)
                pb[j, k, owner] = total.astype(pb.dtype)

            scf(d, k).start()

    def t2(owner, k):
        return tok2.at[k, owner]

    def far2(d, k, owner, target):
        return pltpu.make_async_remote_copy(
            src_ref=t2(owner, k), dst_ref=t2(owner, k), send_sem=g2fs.at[d - 1, k], recv_sem=g2fr.at[d - 1, k],
            device_id={"tp": target}, device_id_type=MESH)

    def near2(d, k, owner):
        return pltpu.make_async_remote_copy(
            src_ref=t2(owner, k), dst_ref=t2(owner, k), send_sem=g2ns.at[d, k], recv_sem=g2nr.at[d, k],
            device_id={"tp": partner}, device_id_type=MESH)

    def mix_end(k):
        scn(0, k).wait_recv()
        for d in range(1, chips):
            scf(d, k).wait_recv()

        @pl.loop(0, r // sub)
        def _(t):
            at = pl.multiple_of(t * sub, sub)
            mid_at = pl.ds(pl.multiple_of(k * r + at, sub), sub)
            power = jnp.zeros((sub, 1), f32)
            mids = []
            for j in range(count):
                total = pb[j, k, me, pl.ds(at, sub), :].astype(f32) + near_in[j, k, pl.ds(at, sub), :].astype(f32)
                for d in range(1, chips):
                    total = total + far_in[d - 1, j, k, pl.ds(at, sub), :].astype(f32)
                cols = slice(j * db, (j + 1) * db)
                middle = (resid[mid_at, cols].astype(f32) + total).astype(out_ref.dtype)
                out_ref[mid_at, cols] = middle
                middle = middle.astype(f32)
                power = power + jnp.sum(middle * middle, axis=-1, keepdims=True)
                mids.append(middle)
            scale = lax.rsqrt(power / width + 1e-06)
            for j in range(count):
                cols = slice(j * db, (j + 1) * db)
                tok2[k, me, pl.ds(at, sub), cols] = (mids[j] * scale * gain2_ref[:, cols]).astype(tok2.dtype)

        for d in range(1, chips):
            far2(d, k, me, chip_core(chip + d, core)).start()
        near2(0, k, me).start()

    def gather_pass(k):
        for d in range(1, chips):
            owner = chip_core(chip - d, core)
            far2(d, k, owner, partner).wait_recv()
            near2(d, k, owner).start()

    for k in range(pieces):
        mix(k)
        if k:
            mix_far(k - 1)
    mix_far(pieces - 1)
    plan = [3, 5, 7, 9]
    for k in range(pieces):
        mix_end(k)
        upto(UP, plan[k * 4 // pieces])
    plan = [10, 12, 13, 14]
    for k in range(pieces):
        gather_pass(k)
        upto(UP, plan[(k + 1) * 4 // pieces - 1])

    for k in range(pieces):
        for d in range(1, chips):
            far1(d, k, me, partner).wait_send()
        for d in range(chips):
            near1(d, k, me).wait_send()
    block = min(512, hid)
    group = n * r

    def expand(k):
        for d in range(chips):
            near2(d, k, chip_core(chip - d, other)).wait_recv()

        @pl.loop(0, hid // block)
        def _(c):
            cols = pl.ds(pl.multiple_of(c * block, block), block)
            lhs = tok2[k].reshape(group, width)
            upper = jnp.dot(lhs, up[:, cols], preferred_element_type=f32)
            upper = jnp.maximum(upper * us_ref[:, cols], 0.0)
            tok1[k * group : (k + 1) * group, cols] = (upper * upper).astype(tok1.dtype)

    for k in range(pieces):
        expand(k)
        upto(DN, k * 4 // pieces)

    for k in range(pieces):
        for d in range(chips):
            scn(d, k).wait_send()
        for d in range(1, chips):
            scf(d, k).wait_send()

    def near(j, d):
        return pltpu.make_async_remote_copy(
            src_ref=pb.at[j, :, chip_core(chip + d, other)], dst_ref=near_in.at[j] if d == 0 else theirs.at[d - 1, j],
            send_sem=mns.at[j, d], recv_sem=mnr.at[j, d], device_id={"tp": partner}, device_id_type=MESH)

    def far(j, d):
        return pltpu.make_async_remote_copy(
            src_ref=pb.at[j, :, chip_core(chip + d, core)], dst_ref=far_in.at[d - 1, j],
            send_sem=mfs.at[j, d - 1], recv_sem=mfr.at[j, d - 1],
            device_id={"tp": chip_core(chip + d, core)}, device_id_type=MESH)

    def contract(j):
        @pl.loop(0, pieces)
        def _(k):
            lhs = tok1[pl.ds(pl.multiple_of(k * group, group), group), 0:hid]
            part = jnp.dot(lhs, dn[j], preferred_element_type=f32)
            pb[j, k] = part.astype(pb.dtype).reshape(n, r, db)

        for d in list(range(1, chips)) + [0]:
            near(j, d).start()

    def combine(j):
        for d in range(1, chips):
            near(j, d).wait_recv()
            owner = chip_core(chip + d, core)

            @pl.loop(0, pieces)
            def _(k):
                total = pb[j, k, owner].astype(f32) + theirs[d - 1, j, k].astype(f32)
                pb[j, k, owner] = total.astype(pb.dtype)

            far(j, d).start()

    def finish(j):
        near(j, 0).wait_recv()
        for d in range(1, chips):
            far(j, d).wait_recv()
        cols = pl.ds(pl.multiple_of(ring_at(pos - j, count) * db, db), db)

        @pl.loop(0, pieces)
        def _(k):
            total = pb[j, k, me].astype(f32) + near_in[j, k].astype(f32)
            for d in range(1, chips):
                total = total + far_in[d - 1, j, k].astype(f32)
            at = pl.ds(pl.multiple_of(k * r, r), r)
            out_ref[at, cols] = (out_ref[at, cols].astype(f32) + total).astype(out_ref.dtype)

    groups = [[0]] + [[s, count - s] if s < far_step else [s] for s in range(1, far_step + 1)]
    for s, slots in enumerate(groups):
        if s:
            for i in range(done[DN], min(s * PIECES, items)):
                service(DN, i)
            done[DN] = max(done[DN], min(s * PIECES, items))
        for j in slots:
            contract(j)
        for j in slots:
            combine(j)
        if s > 1:
            for j in groups[s - 2]:
                finish(j)
    for slots in groups[-2:]:
        for j in slots:
            finish(j)

    for a in range(4):
        for s in range(1, far_step + 1):
            for k in range(PIECES):
                for clockwise in (True, False):
                    if s < far_step or (k < half) == clockwise:
                        hop(a, s, k, clockwise).wait_send()
    for k in range(pieces):
        for d in range(1, chips):
            far2(d, k, me, partner).wait_send()
        for d in range(chips):
            near2(d, k, me).wait_send()
    for j in range(count):
        for d in range(chips):
            near(j, d).wait_send()
        for d in range(1, chips):
            far(j, d).wait_send()


def layer(resid, vg, pt, up, dn, gain1, vs, gs, taps, cgain, gain2, us, n, count, group_width):
    rows, width = resid.shape
    seq = rows * n
    chips = n // CORES
    pieces = CHUNKS // n
    r = rows // pieces
    own_w, db = pt.shape
    hid = dn.shape[0]
    blocks = own_w // LANES
    steps = count // 2
    kind = resid.dtype
    f32 = jnp.float32
    dma = pltpu.SemaphoreType.DMA
    hbm = pl.BlockSpec(memory_space=pl.ANY)
    vmem = pl.BlockSpec(memory_space=pltpu.VMEM)
    return pl.pallas_call(
        functools.partial(layer_kernel, n, count, group_width),
        out_shape=jax.ShapeDtypeStruct(resid.shape, kind),
        in_specs=[hbm] * 5 + [vmem] * 7,
        out_specs=vmem,
        scratch_shapes=[
            pltpu.VMEM((rows, width), kind),
            pltpu.VMEM((seq, max(width, hid)), kind),
            pltpu.VMEM((pieces, n, r, width), kind),
            pltpu.VMEM((width, 2 * own_w), kind),
            pltpu.VMEM((count, own_w, db), kind),
            pltpu.VMEM((width, hid), kind),
            pltpu.VMEM((count, hid, db), kind),
            pltpu.VMEM((blocks, seq + 2 * PAD, LANES), f32),
            pltpu.VMEM((blocks, seq, LANES), f32),
            pltpu.VMEM((seq, own_w), kind),
            pltpu.VMEM((count, pieces, n, r, db), kind),
            pltpu.VMEM((count, pieces, r, db), kind),
            pltpu.VMEM((chips - 1, count, pieces, r, db), kind),
            pltpu.VMEM((chips - 1, count, pieces, r, db), kind),
            pltpu.VMEM((seq // CHUNKS, LANES), f32),
            pltpu.VMEM((n - 1, seq // CHUNKS, LANES), f32),
            dma((5,)),
            dma((4, 2, steps, PIECES)), dma((4, 2, steps, PIECES)),
            dma((chips - 1, pieces)), dma((chips - 1, pieces)), dma((chips, pieces)), dma((chips, pieces)),
            dma((n - 1,)), dma((n - 1,)),
            dma((chips, pieces)), dma((chips, pieces)), dma((chips - 1, pieces)), dma((chips - 1, pieces)),
            dma((chips - 1, pieces)), dma((chips - 1, pieces)), dma((chips, pieces)), dma((chips, pieces)),
            dma((count, chips)), dma((count, chips)), dma((count, chips - 1)), dma((count, chips - 1)),
        ],
        compiler_params=pltpu.CompilerParams(
            collective_id=1, has_side_effects=True, vmem_limit_bytes=67043328
        ),
        cost_estimate=pl.CostEstimate(flops=8 * seq * hid * width, bytes_accessed=8 * seq * width, transcendentals=0),
        name="layer",
    )(resid, vg, pt, up, dn, gain1.reshape(1, -1), vs.reshape(1, -1), gs.reshape(1, -1), taps,
      cgain.reshape(1, -1), gain2.reshape(1, -1), us.reshape(1, -1))


def shards(
    resid,
    norm1_gain,
    w_value,
    w_gate,
    value_scale,
    gate_scale,
    conv_taps,
    conv_gain,
    w_point,
    point_scale,
    norm2_gain,
    w_up,
    up_scale,
    w_down,
    down_scale,
):
    bf = jnp.bfloat16
    vg = jnp.concatenate([w_value.astype(bf), w_gate.astype(bf)], axis=1)
    pt = (w_point * point_scale).astype(bf)
    up = w_up.astype(bf)
    dn = (w_down * down_scale).astype(bf)
    return layer(
        resid, vg, pt, up, dn, norm1_gain, value_scale, gate_scale, conv_taps, conv_gain, norm2_gain, up_scale,
        lax.axis_size("tp"), lax.axis_size("fs"), value_scale.shape[0] // GROUPS,
    )


def solution(mesh):
    in_specs = (
        P(("fs", "tp"), None),
        P(),
        P("fs", "tp"),
        P("fs", "tp"),
        P(),
        P(),
        P(),
        P(),
        P("tp", "fs"),
        P("fs"),
        P(),
        P("fs", "tp"),
        P("tp"),
        P("tp", "fs"),
        P("fs"),
    )
    out_specs = P(("fs", "tp"), None)
    return jax.shard_map(shards, mesh=mesh, in_specs=in_specs, out_specs=out_specs, check_vma=False)
```

```python
import functools

import jax
import jax.numpy as jnp
from jax import lax
from jax.experimental import pallas as pl
from jax.experimental.pallas import tpu as pltpu
from jax.sharding import PartitionSpec as P

GROUPS = 4
CORES = 2
CHUNKS = 16
PIECES = 4
LANES = 128
PAD = 16
MESH = pl.DeviceIdType.MESH


def ring_at(q, count):
    q = lax.rem(q + 2 * count, count)
    high = q // (count // 2)
    return (1 - high) * 2 * q + high * (2 * (count - 1 - q) + 1)


def layer_kernel(
    n, count, group_width,
    resid_hbm, wv_hbm, wg_hbm, wp_hbm, wu_hbm, wd_hbm,
    gain1_hbm, vs_hbm, gs_hbm, taps_hbm, cgain_hbm, ps_hbm, gain2_hbm, us_hbm, ds_hbm,
    out_hbm,
    gain1_ref, vs_ref, gs_ref, taps_ref, cgain_ref, ps_ref, gain2_ref, us_ref, ds_ref,
    mid, store_sem,
    raw_v, raw_g, raw_p, raw_u, raw_d, resid, tok1, tok2, vg, pt, up, dn, gl, cv, act, pb, near_in, far_in, theirs, st, st_in,
    load_sem, ring_send, ring_recv,
    sss, ssr, scns, scnr, scfs, scfr, gfs, gfr, gns, gnr, mns, mnr, mfs, mfr,
):
    me = lax.axis_index("tp")
    core = lax.rem(me, CORES)
    chip = me // CORES
    chips = n // CORES
    other = CORES - 1 - core
    partner = chip * CORES + other
    seat = lax.axis_index("fs")
    odd = lax.rem(seat, 2)
    pos = (1 - odd) * (seat // 2) + odd * (count - 1 - seat // 2)
    right, left = ring_at(pos + 1, count), ring_at(pos - 1, count)
    rows, width = resid.shape
    seq = rows * n
    pieces = CHUNKS // n
    r = rows // pieces
    own_w = pt.shape[1]
    blocks = own_w // LANES
    db = pt.shape[2]
    hid = dn.shape[1]
    far_step = count // 2
    reach = taps_ref.shape[0] // 2
    f32 = jnp.float32

    def chip_core(c, k):
        return lax.rem(c + 2 * chips, chips) * CORES + k

    places = ((wv_hbm, raw_v), (wg_hbm, raw_g), (resid_hbm, resid), (gain1_hbm, gain1_ref),
              (wp_hbm, raw_p), (wu_hbm, raw_u), (wd_hbm, raw_d), (vs_hbm, vs_ref), (gs_hbm, gs_ref),
              (taps_hbm, taps_ref), (cgain_hbm, cgain_ref), (ps_hbm, ps_ref), (gain2_hbm, gain2_ref),
              (us_hbm, us_ref), (ds_hbm, ds_ref))
    loads = [pltpu.make_async_copy(src, dst, load_sem.at[i]) for i, (src, dst) in enumerate(places)]
    for load in loads[:4]:
        load.start()
    barrier = pltpu.get_barrier_semaphore()
    for target in (left, right):
        pl.semaphore_signal(barrier, inc=1, device_id={"fs": target}, device_id_type=MESH)
    for d in range(1, n):
        pl.semaphore_signal(barrier, inc=1, device_id={"tp": lax.rem(me + d, n)}, device_id_type=MESH)

    sub = 16
    own_rows = pl.multiple_of(seat * db, db)
    loads[0].wait()
    loads[1].wait()

    @pl.loop(0, db // sub)
    def _(t):
        src = pl.ds(pl.multiple_of(t * sub, sub), sub)
        dst = pl.ds(pl.multiple_of(own_rows + t * sub, sub), sub)
        vg[dst, 0:own_w] = raw_v[src, :].astype(vg.dtype)
        vg[dst, own_w : 2 * own_w] = raw_g[src, :].astype(vg.dtype)

    for load in loads[4:]:
        load.start()
    pl.semaphore_wait(barrier, n + 1)

    VG, PT, UP, DN = range(4)

    def spot(a, s, k, clockwise):
        owner = ring_at(pos - s if clockwise else pos + s, count)
        if a in (VG, UP):
            step = db // PIECES
            return (vg if a == VG else up).at[pl.ds(pl.multiple_of(owner * db + k * step, step), step)]
        if a == PT:
            step = own_w // PIECES
            return pt.at[owner, pl.ds(pl.multiple_of(k * step, step), step)]
        step = hid // PIECES
        slot = lax.rem(s if clockwise else count - s, count)
        return dn.at[slot, pl.ds(pl.multiple_of(k * step, step), step)]

    def dn_dst(s, k, clockwise):
        step = hid // PIECES
        return dn.at[s if clockwise else count - s, pl.ds(pl.multiple_of(k * step, step), step)]

    def hop(a, s, k, clockwise):
        way = 0 if clockwise else 1
        turn = (s - 1) % 2
        src = spot(a, s - 1, k, clockwise)
        dst = dn_dst(s, k, clockwise) if a == DN else src
        return pltpu.make_async_remote_copy(
            src_ref=src, dst_ref=dst, send_sem=ring_send.at[a % 2, way, turn, k], recv_sem=ring_recv.at[a % 2, way, turn, k],
            device_id={"fs": right if clockwise else left}, device_id_type=MESH)

    def arrived(a, s, k, clockwise):
        way = 0 if clockwise else 1
        turn = (s - 1) % 2
        here = spot(a, s, k, clockwise)
        pltpu.make_async_remote_copy(
            src_ref=here, dst_ref=here, send_sem=ring_send.at[a % 2, way, turn, k], recv_sem=ring_recv.at[a % 2, way, turn, k],
            device_id={"fs": right if clockwise else left}, device_id_type=MESH).wait_recv()

    half = PIECES // 2
    full_items = (far_step - 1) * PIECES
    items = full_items + half

    def first_hop(a, k):
        if a >= 2:
            drain(a - 2, k)
        for clockwise in (True, False):
            hop(a, 1, k, clockwise).start()

    def first_hops(a):
        for k in range(PIECES):
            first_hop(a, k)

    def drain(a, k):
        for clockwise in (True, False):
            last_step = far_step if (k < half) == clockwise else far_step - 1
            for s in range(max(1, last_step - 1), last_step + 1):
                hop(a, s, k, clockwise).wait_send()

    def service(a, i):
        if isinstance(i, int) and i >= full_items:
            k = i - full_items
            arrived(a, far_step, k, True)
            arrived(a, far_step, k + half, False)
            return
        s, k = i // PIECES + 1, i % PIECES
        for clockwise in (True, False):
            arrived(a, s, k, clockwise)
        for clockwise in (True, False):
            mine = k < half if clockwise else k >= half
            if isinstance(i, int):
                if s + 1 < far_step or mine:
                    if s > 1:
                        hop(a, s - 1, k, clockwise).wait_send()
                    hop(a, s + 1, k, clockwise).start()
            else:
                @pl.when(jnp.logical_and(s > 1, jnp.logical_or(s + 1 < far_step, mine)))
                def _():
                    hop(a, s - 1, k, clockwise).wait_send()

                @pl.when(jnp.logical_or(s + 1 < far_step, mine))
                def _():
                    hop(a, s + 1, k, clockwise).start()

    done = [0, 0, 0, 0]

    def upto(a, q):
        q = q * items // 14
        for i in range(done[a], q):
            service(a, i)
            if i == full_items - 1 and a < DN:
                first_hops(a + 1)
        done[a] = max(done[a], q)

    first_hops(VG)

    loads[2].wait()
    loads[3].wait()

    def t1(owner, k):
        return tok1.at[pl.ds(pl.multiple_of(owner * rows + k * r, r), r)]

    def far1(d, k, owner, target):
        return pltpu.make_async_remote_copy(
            src_ref=t1(owner, k), dst_ref=t1(owner, k), send_sem=gfs.at[d - 1, k], recv_sem=gfr.at[d - 1, k],
            device_id={"tp": target}, device_id_type=MESH)

    def near1(d, k, owner):
        return pltpu.make_async_remote_copy(
            src_ref=t1(owner, k), dst_ref=t1(owner, k), send_sem=gns.at[d, k], recv_sem=gnr.at[d, k],
            device_id={"tp": partner}, device_id_type=MESH)

    for k in range(pieces):
        @pl.loop(0, r // sub)
        def _(t):
            at = k * r + t * sub
            data = resid[pl.ds(pl.multiple_of(at, sub), sub), :].astype(f32)
            scale = lax.rsqrt(jnp.mean(data * data, axis=-1, keepdims=True) + 1e-06)
            tok1[pl.ds(pl.multiple_of(me * rows + at, sub), sub), :] = (data * scale * gain1_ref[...]).astype(tok1.dtype)

        for d in range(1, chips):
            far1(d, k, me, chip_core(chip + d, core)).start()
        near1(0, k, me).start()
    for load in loads[4:]:
        load.wait()

    @pl.loop(0, own_w // sub)
    def _(t):
        at = pl.ds(pl.multiple_of(t * sub, sub), sub)
        pt[seat, at, :] = (raw_p[at, :] * ps_ref[...]).astype(pt.dtype)

    @pl.loop(0, db // sub)
    def _(t):
        up[pl.ds(pl.multiple_of(own_rows + t * sub, sub), sub), :] = raw_u[
            pl.ds(pl.multiple_of(t * sub, sub), sub), :].astype(up.dtype)

    @pl.loop(0, hid // sub)
    def _(t):
        at = pl.ds(pl.multiple_of(t * sub, sub), sub)
        dn[0, at, :] = (raw_d[at, :] * ds_ref[...]).astype(dn.dtype)

    passed = 0
    for q in range(14):
        upto(VG, q + 1)
        while passed < pieces and (passed + 1) * 13 // pieces <= q + 1:
            for d in range(1, chips):
                owner = chip_core(chip - d, core)
                far1(d, passed, owner, partner).wait_recv()
                near1(d, passed, owner).start()
            passed += 1
    for k in range(pieces):
        for d in range(chips):
            near1(d, k, chip_core(chip - d, other)).wait_recv()

    gl[:, 0:PAD, :] = jnp.zeros((blocks, PAD, LANES), f32)
    gl[:, PAD + seq :, :] = jnp.zeros((blocks, PAD, LANES), f32)
    mine_w = pl.multiple_of(me * own_w, own_w)
    tile = 256
    tiles = seq // tile
    wide = 2 * LANES

    @pl.loop(0, tiles)
    def _(t):
        at = pl.multiple_of(t * tile, tile)
        for c in range(0, own_w, wide):
            lhs = tok1[pl.ds(at, tile), :]
            value = jnp.dot(lhs, vg[:, c : c + wide], preferred_element_type=f32)
            gate = jnp.dot(lhs, vg[:, own_w + c : own_w + c + wide], preferred_element_type=f32)
            value = value * vs_ref[:, pl.ds(mine_w + c, wide)]
            gate = gate * gs_ref[:, pl.ds(mine_w + c, wide)]
            glu = (value * jax.nn.sigmoid(gate)).astype(jnp.bfloat16).astype(f32)
            for b in range(wide // LANES):
                gl[c // LANES + b, pl.ds(PAD + at, tile), :] = glu[:, b * LANES : (b + 1) * LANES]

        @pl.when(jnp.logical_and(t >= 1, t < 2 + PIECES))
        def _():
            service(PT, t - 1)

    done[PT] = PIECES + 1

    span = seq // CHUNKS
    lane = lax.broadcasted_iota(jnp.int32, (span, LANES), 1)
    st[...] = jnp.zeros(st.shape, f32)

    def spread(v, width_from):
        while width_from < LANES:
            v = v + pltpu.roll(v, width_from, 1)
            width_from *= 2
        return v

    @pl.loop(0, CHUNKS)
    def _(i):
        at = pl.multiple_of(i * span, span)
        total = jnp.zeros((span, LANES), f32)
        square = jnp.zeros((span, LANES), f32)
        for b in range(blocks):
            window = gl[b, pl.ds(at, span + 2 * PAD), :]
            lanes = pl.ds(mine_w + b * LANES, LANES)
            conv = None
            for phase in range(8):
                acc = None
                for a in range(4):
                    j = 8 * a + phase + reach - PAD
                    if j < 0 or j > 2 * reach:
                        continue
                    term = taps_ref[j : j + 1, lanes] * window[8 * a : 8 * a + span + 8]
                    acc = term if acc is None else acc + term
                if phase:
                    acc = pltpu.roll(acc, span + 8 - phase, 0)
                acc = acc[:span]
                conv = acc if conv is None else conv + acc
            cv[b, pl.ds(at, span), :] = conv
            total = total + conv
            square = square + conv * conv
        total = spread(total, GROUPS)
        square = spread(square, GROUPS)
        here = lane // (2 * GROUPS) == i
        st[...] = jnp.where(here, jnp.where(lane % (2 * GROUPS) < GROUPS, total, square), st[...])

        @pl.when(jnp.logical_and(i < 11, i % 3 > 0))
        def _():
            service(PT, PIECES + i // 3 * 2 + i % 3)

        if full_items == 3 * PIECES:
            @pl.when(i == 10)
            def _():
                first_hops(UP)

    done[PT] = 3 * PIECES

    def stat(d):
        return pltpu.make_async_remote_copy(
            src_ref=st, dst_ref=st_in.at[d - 1], send_sem=sss.at[d - 1], recv_sem=ssr.at[d - 1],
            device_id={"tp": lax.rem(me + d, n)}, device_id_type=MESH)

    for d in range(1, n):
        stat(d).start()
    upto(PT, 14)
    for k in range(pieces):
        for d in range(1, chips):
            far1(d, k, me, partner).wait_send()
        for d in range(chips):
            near1(d, k, me).wait_send()
    for d in range(1, n):
        stat(d).wait_recv()
    for d in range(1, n):
        stat(d).wait_send()
    st_sum = st[...]
    for d in range(1, n):
        st_sum = st_sum + st_in[d - 1]
    st[...] = st_sum

    def scn(d, k):
        return pltpu.make_async_remote_copy(
            src_ref=pb.at[:, k, chip_core(chip + d, other)],
            dst_ref=near_in.at[:, k] if d == 0 else theirs.at[d - 1, :, k],
            send_sem=scns.at[d, k], recv_sem=scnr.at[d, k], device_id={"tp": partner}, device_id_type=MESH)

    def scf(d, k):
        return pltpu.make_async_remote_copy(
            src_ref=pb.at[:, k, chip_core(chip + d, core)], dst_ref=far_in.at[d - 1, :, k],
            send_sem=scfs.at[d - 1, k], recv_sem=scfr.at[d - 1, k],
            device_id={"tp": chip_core(chip + d, core)}, device_id_type=MESH)

    def mix(k):
        @pl.loop(0, n)
        def _(o):
            i = o * pieces + k
            here = lane // GROUPS
            stats = st[...]
            gmean = spread(jnp.where(here == 2 * i, stats, 0.0), GROUPS) / group_width
            gsquare = spread(jnp.where(here == 2 * i + 1, stats, 0.0), GROUPS) / group_width
            inv = lax.rsqrt(gsquare - gmean * gmean + 1e-05)
            for b in range(blocks):
                conv = cv[b, pl.ds(pl.multiple_of(i * span, span), span), :]
                scaled = (conv - gmean) * inv * cgain_ref[:, pl.ds(mine_w + b * LANES, LANES)]
                act[pl.ds(pl.multiple_of((k * n + o) * r, r), r), b * LANES : (b + 1) * LANES] = (
                    scaled / (1.0 + jnp.exp(-scaled))
                ).astype(act.dtype)

        @pl.loop(0, count)
        def _(j):
            part = jnp.dot(act[k * n * r : (k + 1) * n * r, :], pt[j], preferred_element_type=f32)
            pb[j, k] = part.astype(pb.dtype).reshape(n, r, db)

        for d in list(range(1, chips)) + [0]:
            scn(d, k).start()

    def mix_far(k):
        for d in range(1, chips):
            scn(d, k).wait_recv()
            owner = chip_core(chip + d, core)

            @pl.loop(0, count)
            def _(j):
                total = pb[j, k, owner].astype(f32) + theirs[d - 1, j, k].astype(f32)
                pb[j, k, owner] = total.astype(pb.dtype)

            scf(d, k).start()

    def t2(owner, k):
        return tok2.at[k, owner]

    def far2(d, k, owner, target):
        return pltpu.make_async_remote_copy(
            src_ref=t2(owner, k), dst_ref=t2(owner, k), send_sem=gfs.at[d - 1, k], recv_sem=gfr.at[d - 1, k],
            device_id={"tp": target}, device_id_type=MESH)

    def near2(d, k, owner):
        return pltpu.make_async_remote_copy(
            src_ref=t2(owner, k), dst_ref=t2(owner, k), send_sem=gns.at[d, k], recv_sem=gnr.at[d, k],
            device_id={"tp": partner}, device_id_type=MESH)

    def mix_end(k):
        scn(0, k).wait_recv()
        for d in range(1, chips):
            scf(d, k).wait_recv()

        @pl.loop(0, r // sub)
        def _(t):
            at = pl.multiple_of(t * sub, sub)
            mid_at = pl.ds(pl.multiple_of(k * r + at, sub), sub)
            power = jnp.zeros((sub, 1), f32)
            mids = []
            for j in range(count):
                total = pb[j, k, me, pl.ds(at, sub), :].astype(f32) + near_in[j, k, pl.ds(at, sub), :].astype(f32)
                for d in range(1, chips):
                    total = total + far_in[d - 1, j, k, pl.ds(at, sub), :].astype(f32)
                cols = slice(j * db, (j + 1) * db)
                middle = (resid[mid_at, cols].astype(f32) + total).astype(mid.dtype)
                mid[mid_at, cols] = middle
                middle = middle.astype(f32)
                power = power + jnp.sum(middle * middle, axis=-1, keepdims=True)
                mids.append(middle)
            scale = lax.rsqrt(power / width + 1e-06)
            for j in range(count):
                cols = slice(j * db, (j + 1) * db)
                tok2[k, me, pl.ds(at, sub), cols] = (mids[j] * scale * gain2_ref[:, cols]).astype(tok2.dtype)

        for d in range(1, chips):
            far2(d, k, me, chip_core(chip + d, core)).start()
        near2(0, k, me).start()

    def gather_pass(k):
        for d in range(1, chips):
            owner = chip_core(chip - d, core)
            far2(d, k, owner, partner).wait_recv()
            near2(d, k, owner).start()

    for k in range(pieces):
        mix(k)
        if k:
            mix_far(k - 1)
        upto(UP, min(k * 4 // pieces + 1, 3))
    mix_far(pieces - 1)
    plan = [4, 6, 7, 9]
    for k in range(pieces):
        mix_end(k)
        upto(UP, plan[k * 4 // pieces])
    block = min(512, hid)
    group = n * r

    def expand(k):
        for d in range(chips):
            near2(d, k, chip_core(chip - d, other)).wait_recv()

        @pl.loop(0, hid // block)
        def _(c):
            cols = pl.ds(pl.multiple_of(c * block, block), block)
            lhs = tok2[k].reshape(group, width)
            upper = jnp.dot(lhs, up[:, cols], preferred_element_type=f32)
            upper = jnp.maximum(upper * us_ref[:, cols], 0.0)
            tok1[k * group : (k + 1) * group, cols] = (upper * upper).astype(tok1.dtype)

    plan = [10, 12, 14, 14]
    for k in range(pieces):
        gather_pass(k)
        upto(UP, plan[(k + 1) * 4 // pieces - 1])
        if k == pieces - 2:
            expand(0)
    for k in range(1 if pieces > 1 else 0, pieces):
        expand(k)
        upto(DN, k * 4 // pieces)

    for k in range(pieces):
        for d in range(chips):
            scn(d, k).wait_send()
        for d in range(1, chips):
            scf(d, k).wait_send()

    def near(j, d):
        return pltpu.make_async_remote_copy(
            src_ref=pb.at[j, :, chip_core(chip + d, other)], dst_ref=near_in.at[j] if d == 0 else theirs.at[d - 1, j],
            send_sem=mns.at[j, d], recv_sem=mnr.at[j, d], device_id={"tp": partner}, device_id_type=MESH)

    def far(j, d):
        return pltpu.make_async_remote_copy(
            src_ref=pb.at[j, :, chip_core(chip + d, core)], dst_ref=far_in.at[d - 1, j],
            send_sem=mfs.at[j, d - 1], recv_sem=mfr.at[j, d - 1],
            device_id={"tp": chip_core(chip + d, core)}, device_id_type=MESH)

    def contract(j):
        @pl.loop(0, pieces)
        def _(k):
            lhs = tok1[pl.ds(pl.multiple_of(k * group, group), group), 0:hid]
            part = jnp.dot(lhs, dn[j], preferred_element_type=f32)
            pb[j, k] = part.astype(pb.dtype).reshape(n, r, db)

        for d in list(range(1, chips)) + [0]:
            near(j, d).start()

    def combine(j):
        for d in range(1, chips):
            near(j, d).wait_recv()
            owner = chip_core(chip + d, core)

            @pl.loop(0, pieces)
            def _(k):
                total = pb[j, k, owner].astype(f32) + theirs[d - 1, j, k].astype(f32)
                pb[j, k, owner] = total.astype(pb.dtype)

            far(j, d).start()

    def finish(j):
        near(j, 0).wait_recv()
        for d in range(1, chips):
            far(j, d).wait_recv()
        cols = pl.ds(pl.multiple_of(ring_at(pos - j, count) * db, db), db)

        @pl.loop(0, pieces)
        def _(k):
            total = pb[j, k, me].astype(f32) + near_in[j, k].astype(f32)
            for d in range(1, chips):
                total = total + far_in[d - 1, j, k].astype(f32)
            at = pl.ds(pl.multiple_of(k * r, r), r)
            mid[at, cols] = (mid[at, cols].astype(f32) + total).astype(mid.dtype)

    last = far_step

    def near_last(k, d):
        return pltpu.make_async_remote_copy(
            src_ref=pb.at[last, k, chip_core(chip + d, other)],
            dst_ref=near_in.at[last, k] if d == 0 else theirs.at[d - 1, last, k],
            send_sem=scns.at[d, k], recv_sem=scnr.at[d, k], device_id={"tp": partner}, device_id_type=MESH)

    def far_last(k, d):
        return pltpu.make_async_remote_copy(
            src_ref=pb.at[last, k, chip_core(chip + d, core)], dst_ref=far_in.at[d - 1, last, k],
            send_sem=scfs.at[d - 1, k], recv_sem=scfr.at[d - 1, k],
            device_id={"tp": chip_core(chip + d, core)}, device_id_type=MESH)

    def contract_last(k):
        lhs = tok1[k * group : (k + 1) * group, 0:hid]
        part = jnp.dot(lhs, dn[last], preferred_element_type=f32)
        pb[last, k] = part.astype(pb.dtype).reshape(n, r, db)
        for d in list(range(1, chips)) + [0]:
            near_last(k, d).start()

    def combine_last(k):
        for d in range(1, chips):
            near_last(k, d).wait_recv()
            owner = chip_core(chip + d, core)
            total = pb[last, k, owner].astype(f32) + theirs[d - 1, last, k].astype(f32)
            pb[last, k, owner] = total.astype(pb.dtype)
            far_last(k, d).start()

    def finish_last(k):
        near_last(k, 0).wait_recv()
        for d in range(1, chips):
            far_last(k, d).wait_recv()
        cols = pl.ds(pl.multiple_of(ring_at(pos - last, count) * db, db), db)
        total = pb[last, k, me].astype(f32) + near_in[last, k].astype(f32)
        for d in range(1, chips):
            total = total + far_in[d - 1, last, k].astype(f32)
        at = slice(k * r, (k + 1) * r)
        mid[at, cols] = (mid[at, cols].astype(f32) + total).astype(mid.dtype)

    def slots_sent(slots):
        for j in slots:
            for d in range(chips):
                near(j, d).wait_send()
            for d in range(1, chips):
                far(j, d).wait_send()

    def store(j):
        cols = pl.ds(pl.multiple_of(ring_at(pos - j, count) * db, db), db)
        return pltpu.make_async_copy(mid.at[:, cols], out_hbm.at[:, cols], store_sem.at[j])

    groups = [[0]] + [[s, count - s] for s in range(1, far_step)]
    for s, slots in enumerate(groups):
        if s:
            for i in range(done[DN], min(s * PIECES, items)):
                service(DN, i)
            done[DN] = max(done[DN], min(s * PIECES, items))
        for j in slots:
            contract(j)
        for j in slots:
            combine(j)
        if s > 1:
            for j in groups[s - 2]:
                finish(j)
                store(j).start()
        if s == 1:
            for k in range(PIECES):
                drain(UP, k)
            for k in range(pieces):
                for d in range(1, chips):
                    far2(d, k, me, partner).wait_send()
                for d in range(chips):
                    near2(d, k, me).wait_send()
    for j in groups[-2]:
        finish(j)
        store(j).start()
    upto(DN, 13)
    for slots in groups[:-1]:
        slots_sent(slots)
    upto(DN, 14)
    for k in range(pieces):
        contract_last(k)
        if k:
            combine_last(k - 1)
    combine_last(pieces - 1)
    for j in groups[-1]:
        finish(j)
        store(j).start()
    for k in range(pieces):
        finish_last(k)
    store(last).start()

    for k in range(PIECES):
        drain(DN, k)
    slots_sent(groups[-1])
    for k in range(pieces):
        for d in range(chips):
            near_last(k, d).wait_send()
        for d in range(1, chips):
            far_last(k, d).wait_send()
    for j in range(count):
        store(j).wait()


def layer(resid, wv, wg, wp, wu, wd, gain1, vs, gs, taps, cgain, ps, gain2, us, ds, n, count, group_width):
    rows, width = resid.shape
    seq = rows * n
    chips = n // CORES
    pieces = CHUNKS // n
    r = rows // pieces
    own_w, db = wp.shape
    hid = wd.shape[0]
    blocks = own_w // LANES
    kind = resid.dtype
    f32 = jnp.float32
    dma = pltpu.SemaphoreType.DMA
    hbm = pl.BlockSpec(memory_space=pl.ANY)
    small = (
        gain1.reshape(1, -1), vs.reshape(1, -1), gs.reshape(1, -1), taps, cgain.reshape(1, -1), ps.reshape(1, -1),
        gain2.reshape(1, -1), us.reshape(1, -1), ds.reshape(1, -1),
    )
    return pl.pallas_call(
        functools.partial(layer_kernel, n, count, group_width),
        out_shape=jax.ShapeDtypeStruct(resid.shape, kind),
        in_specs=[hbm] * 15,
        out_specs=hbm,
        scratch_shapes=[
            *(pltpu.VMEM(x.shape, x.dtype) for x in small),
            pltpu.VMEM((rows, width), kind),
            dma((count,)),
            pltpu.VMEM((db, own_w), f32),
            pltpu.VMEM((db, own_w), f32),
            pltpu.VMEM((own_w, db), f32),
            pltpu.VMEM((db, hid), f32),
            pltpu.VMEM((hid, db), f32),
            pltpu.VMEM((rows, width), kind),
            pltpu.VMEM((seq, max(width, hid)), kind),
            pltpu.VMEM((pieces, n, r, width), kind),
            pltpu.VMEM((width, 2 * own_w), kind),
            pltpu.VMEM((count, own_w, db), kind),
            pltpu.VMEM((width, hid), kind),
            pltpu.VMEM((count, hid, db), kind),
            pltpu.VMEM((blocks, seq + 2 * PAD, LANES), f32),
            pltpu.VMEM((blocks, seq, LANES), f32),
            pltpu.VMEM((seq, own_w), kind),
            pltpu.VMEM((count, pieces, n, r, db), kind),
            pltpu.VMEM((count, pieces, r, db), kind),
            pltpu.VMEM((chips - 1, count, pieces, r, db), kind),
            pltpu.VMEM((chips - 1, count, pieces, r, db), kind),
            pltpu.VMEM((seq // CHUNKS, LANES), f32),
            pltpu.VMEM((n - 1, seq // CHUNKS, LANES), f32),
            dma((15,)),
            dma((2, 2, 2, PIECES)), dma((2, 2, 2, PIECES)),
            dma((n - 1,)), dma((n - 1,)),
            dma((chips, pieces)), dma((chips, pieces)), dma((chips - 1, pieces)), dma((chips - 1, pieces)),
            dma((chips - 1, pieces)), dma((chips - 1, pieces)), dma((chips, pieces)), dma((chips, pieces)),
            dma((count, chips)), dma((count, chips)), dma((count, chips - 1)), dma((count, chips - 1)),
        ],
        compiler_params=pltpu.CompilerParams(
            collective_id=1, has_side_effects=True, vmem_limit_bytes=67043328
        ),
        cost_estimate=pl.CostEstimate(flops=8 * seq * hid * width, bytes_accessed=8 * seq * width, transcendentals=0),
        name="layer",
    )(resid, wv, wg, wp, wu, wd, *small)


def shards(
    resid,
    norm1_gain,
    w_value,
    w_gate,
    value_scale,
    gate_scale,
    conv_taps,
    conv_gain,
    w_point,
    point_scale,
    norm2_gain,
    w_up,
    up_scale,
    w_down,
    down_scale,
):
    return layer(
        resid, w_value, w_gate, w_point, w_up, w_down,
        norm1_gain, value_scale, gate_scale, conv_taps, conv_gain, point_scale, norm2_gain, up_scale, down_scale,
        lax.axis_size("tp"), lax.axis_size("fs"), value_scale.shape[0] // GROUPS,
    )


def solution(mesh):
    in_specs = (
        P(("fs", "tp"), None),
        P(),
        P("fs", "tp"),
        P("fs", "tp"),
        P(),
        P(),
        P(),
        P(),
        P("tp", "fs"),
        P("fs"),
        P(),
        P("fs", "tp"),
        P("tp"),
        P("tp", "fs"),
        P("fs"),
    )
    out_specs = P(("fs", "tp"), None)
    return jax.shard_map(shards, mesh=mesh, in_specs=in_specs, out_specs=out_specs, check_vma=False)
```
